32 devices in a mesh: sp: 16 (over z, y, core), tp: 2 (over x).
Axes of the slice: x: 2, y: 2, z: 4, core: 2. Of those that a mesh axis runs over, the one named last changes fastest.
Arguments:
- queries: bfloat16 [8192, 1024], P('sp', 'tp'), may hold values from -40 to 40
- keys_values: bfloat16 [8192, 4, 128], P('sp', 'tp'), may hold values from -40 to 40
- doc_ids: int32 [8192], P('sp'), may hold values from 0 to 3, never falling along the last dimension, each value on 1 to 4096 neighbouring positions
- head_sink: float32 [16], P('tp'), may hold values from 3 to 7
- out_weight: bfloat16 [1024, 2048], replicated, may hold values from -0.1875 to 0.1875
- hidden_in: bfloat16 [8192, 2048], P(('sp', 'tp')), may hold values from -0.59765625 to 0.59765625
- norm_gain: float32 [2048], replicated, may hold values from 0.1 to 1.9
- expert_gate: bfloat16 [32, 2048, 1024], P(('sp', 'tp')), may hold values from -0.125 to 0.125
- expert_up: bfloat16 [32, 2048, 1024], P(('sp', 'tp')), may hold values from -0.125 to 0.125
- expert_down: bfloat16 [32, 1024, 2048], P(('sp', 'tp')), may hold values from -0.1875 to 0.1875
- routes: int32 [8192, 2], P(('sp', 'tp')), may hold values from 0 to 31, all different within a row; in each aligned block of 256 rows (0 to 255, 256 to 511, ...) at most 32 rows name the same one
- route_weight: float32 [8192, 2], P(('sp', 'tp')), may hold values from 0.1 to 1
Outputs:
- layer_out: bfloat16 [8192, 2048], P(('sp', 'tp'))
The draws below stay inside these ranges and needn't reach their ends.
Inputs may be any that keep to these rules, and one draw needn't show every extreme that they name: `routes`: in the rows of one device (aligned blocks of 256 tokens in order) no expert is named more than 32 times; some expert is named exactly 32 times in some blocks.
All inputs are finite; a program needn't handle non-finite values.
Results may differ from the reference program's by a relative error of at most 0.02.
Values may be sent and summed in bfloat16 or wider, within the bound.
No kernel may reach another device: no remote copies, remote signals or barrier semaphores. Data moves between devices by JAX's collectives and lax.ppermute only.
A program may use at most 64 MiB of HBM per device.

```python
import math
import jax
import jax.numpy as jnp
import numpy as np
from jax import lax

D = 2048
HQ = 16
KVH = 4
HD = 64
FF = 1024
TOPK = 2
WIN = 128
TOK_DEV = 512
TOKENS = 8192
EXPERTS = 32
CAP = 32
DOCS = 4
N_TP = 2


def drawn_pair(key):
    base = jax.random.fold_in(key, 11)
    query_key, pair_key = jax.random.split(base, 2)
    queries = jnp.clip(jax.random.normal(query_key, (TOKENS, HQ * HD), jnp.float32), -6.0, 6.0)
    pairs = jnp.clip(jax.random.normal(pair_key, (TOKENS, KVH, 2 * HD), jnp.float32), -6.0, 6.0)
    return (queries, pairs)


def draw_queries(key, part):
    return drawn_pair(key)[0].astype(jnp.bfloat16)


def draw_keys_values(key, part):
    return drawn_pair(key)[1].astype(jnp.bfloat16)


def level_of(own_key, shape, shards, smallest, largest):
    factor_of = 1.0
    for dim, shards_of in shards:
        steps = jax.random.uniform(jax.random.fold_in(jax.random.fold_in(own_key, 6), dim), (shards_of,), jnp.float32, smallest / len(shards), largest / len(shards))
        factor_of = factor_of * jnp.repeat(jnp.exp(steps), shape[dim] // shards_of).reshape((-1,) + (1,) * (len(shape) - 1 - dim))
    return factor_of


def length_profile(number_of, total, most, slope):
    weights = [(1 << 20) // math.isqrt(rank ** slope) + 1 for rank in range(2, number_of + 1)]
    spare, given = total - most - (number_of - 1), [1] * (number_of - 1)
    while spare > 0:
        candidates = [i for i in range(number_of - 1) if given[i] < most]
        mass, left = sum([weights[i] for i in candidates]), spare
        for i in candidates:
            extra = min(most - given[i], max(1, left * weights[i] // mass), spare)
            given[i] = given[i] + extra
            spare = spare - extra
    return np.array([most] + given)


def ragged_sizes(stream_key, amount, total, most, skew):
    if amount == 2:
        one = jax.random.randint(stream_key, (), max(1, total - most), min(most, total - 1) + 1)
        return jnp.stack([one, total - one])
    tallies = jnp.asarray(length_profile(amount, total, most, skew), jnp.int32)
    pairs = (amount - 1) // 2
    donor, taker = tallies[1:1 + 2 * pairs:2], tallies[2:2 + 2 * pairs:2]
    room = jnp.minimum(donor - 1, most - taker)
    moved = jax.random.randint(jax.random.fold_in(stream_key, 1), (pairs,), 0, 1 << 20) % (room + 1)
    tallies = tallies.at[1:1 + 2 * pairs:2].set(donor - moved).at[2:2 + 2 * pairs:2].set(taker + moved)
    return tallies[jax.random.permutation(jax.random.fold_in(stream_key, 2), amount)]


def assign_block(key, own, number, rows, amount, top, limit, lean):
    sequence = jax.random.permutation(key, amount)
    heavy_load, common = load_shares(amount, rows * top, limit, lean, True), load_shares(amount, rows * top, limit, lean, False)
    places = jnp.arange(amount)

    def named(sizes, rotation):
        used = int((sizes > 0).sum())
        fixed = max(1, used // 4)
        passed = fixed + (places - fixed + rotation * (used - fixed)) % max(1, amount - fixed)
        return jnp.zeros((amount,), jnp.int32).at[sequence[jnp.where(places < fixed, places, passed)]].set(jnp.asarray(sizes, jnp.int32))

    sizes = jnp.where(number % 4 == 0, named(heavy_load, number // 4), named(common, number - number // 4 - 1))
    mixed = jax.random.permutation(jax.random.fold_in(own, 3), amount)
    source_of, receiver = mixed[0:amount // 2 * 2:2], mixed[1:amount // 2 * 2:2]
    slack = jnp.minimum(sizes[source_of] - 1, limit - sizes[receiver]) // 2
    slack = jnp.where((source_of == sequence[0]) | (receiver == sequence[0]) | (sizes[receiver] == 0), 0, jnp.maximum(slack, 0))
    passed = jax.random.randint(jax.random.fold_in(own, 4), (amount // 2,), 0, 1 << 20) % (slack + 1)
    sizes = sizes.at[source_of].add(-passed).at[receiver].add(passed)
    members = jnp.searchsorted(jnp.cumsum(sizes), jnp.arange(rows * top), side="right").astype(jnp.int32)
    grid = members.reshape(top, rows).T
    grid = grid[jax.random.permutation(jax.random.fold_in(own, 1), rows)]
    rotation = jax.random.randint(jax.random.fold_in(own, 2), (rows, 1), 0, top)
    return jnp.take_along_axis(grid, (jnp.arange(top)[None, :] + rotation) % top, axis=1)


def load_shares(amount, total, bound, lean, full):
    portions = [(1 << 20) // math.isqrt(standing ** lean) + 1 for standing in range(1, amount + 1)]
    largest = bound if full else min(bound, max(-(-total // amount), total * portions[0] // sum(portions)))
    least = 1 if total - largest >= amount - 1 else 0
    counts, surplus = [largest] + [least] * (amount - 1), total - largest - least * (amount - 1)
    while surplus > 0:
        candidates = [i for i in range(1, amount) if counts[i] < largest] or [i for i in range(1, amount) if counts[i] < bound]
        whole, remaining = sum([portions[i] for i in candidates]), surplus
        for i in candidates:
            extra = min(bound - counts[i], max(1, remaining * portions[i] // whole), surplus)
            counts[i] = counts[i] + extra
            surplus = surplus - extra
    return np.array(counts)


def normal_values(stream_key, shape, spread, reach, cuts=(), held_as=jnp.bfloat16):
    drawn = jax.random.normal(stream_key, shape, jnp.float32) * spread
    if len(cuts) > 0:
        drawn = level_of(stream_key, shape, cuts, -0.22, 0.18) * drawn
    return jnp.clip(drawn, min=-reach, max=reach).astype(held_as)


def setup_inputs(seed: int = 0) -> dict:
    seeds = jax.random.split(jax.random.key(seed), 13)
    queries = draw_queries(jax.random.fold_in(seeds[12], 71), 0)
    keys_values = draw_keys_values(jax.random.fold_in(seeds[12], 71), 0)
    doc_ids = jnp.searchsorted(jnp.cumsum(ragged_sizes(seeds[2], DOCS, TOKENS, 8 * TOK_DEV, 1)), jnp.arange(TOKENS), side="right").astype(jnp.int32)
    head_sink = jnp.clip(3.0 + 4.0 * jax.random.uniform(seeds[3], (HQ,), jnp.float32) ** level_of(seeds[3], (HQ,), ((0, 2),), -0.2, 0.2), 3.0, 7.0)
    out_weight = normal_values(seeds[4], (HQ * HD, D), (HQ * HD) ** -0.5, 0.1875)
    hidden_in = normal_values(seeds[5], (TOKENS, D), 0.1, 0.59765625, ((0, 32),))
    norm_gain = jnp.clip(1.0 + 0.18 * jax.random.normal(seeds[6], (D,), jnp.float32), 0.1, 1.9)
    expert_gate = normal_values(seeds[7], (EXPERTS, D, FF), D ** -0.5, 0.125, ((0, 32),))
    expert_up = normal_values(seeds[8], (EXPERTS, D, FF), D ** -0.5, 0.125, ((0, 32),))
    expert_down = normal_values(seeds[9], (EXPERTS, FF, D), FF ** -0.5, 0.1875, ((0, 32),))
    routes_keys = jax.random.split(jax.random.fold_in(seeds[10], 1), TOKENS // (TOK_DEV // N_TP))
    routes_turns = jax.random.permutation(jax.random.fold_in(seeds[10], 3), TOKENS // (TOK_DEV // N_TP))
    routes = jax.vmap(lambda own, number: assign_block(jax.random.fold_in(seeds[10], 2), own, number, TOK_DEV // N_TP, EXPERTS, TOPK, CAP, 1))(routes_keys, routes_turns).reshape((TOKENS, TOPK))
    route_weight = jnp.clip(jnp.exp(math.log(1.0) - 2.3025851 * jax.random.uniform(seeds[11], (TOKENS, TOPK), jnp.float32) ** level_of(seeds[11], (TOKENS, TOPK), ((0, 32),), -0.2, 0.2)), 0.1, 1.0)
    return {"queries": queries, "keys_values": keys_values, "doc_ids": doc_ids, "head_sink": head_sink, "out_weight": out_weight, "hidden_in": hidden_in, "norm_gain": norm_gain, "expert_gate": expert_gate, "expert_up": expert_up, "expert_down": expert_down, "routes": routes, "route_weight": route_weight}


def attend_all(queries, keys_values, doc_ids, head_sink):
    span_rows = math.gcd(512, TOKENS)
    span_count = TOKENS // span_rows
    group = HQ // KVH
    padded = jnp.pad(keys_values, ((WIN, WIN), (0, 0), (0, 0)))
    padded_docs = jnp.pad(doc_ids, (WIN, WIN), constant_values=-1)
    sink_logit = head_sink.astype(jnp.float32).reshape(KVH, group)[:, :, None, None]

    def one_span(span_index):
        first_row = (span_index * span_rows).astype(jnp.int32)
        q_span = lax.dynamic_slice_in_dim(queries, first_row, span_rows, 0).astype(jnp.float32)
        q_span = q_span.reshape(span_rows, KVH, group, HD)
        kv_span = lax.dynamic_slice_in_dim(padded, first_row, span_rows + 2 * WIN, 0).astype(jnp.float32)
        key_docs = lax.dynamic_slice_in_dim(padded_docs, first_row, span_rows + 2 * WIN, 0)
        query_docs = lax.dynamic_slice_in_dim(doc_ids, first_row, span_rows, 0)
        scores = jnp.einsum('qhgd,khd->hgqk', q_span, kv_span[..., :HD]) * HD ** (-0.5)
        query_pos = first_row + jnp.arange(span_rows, dtype=jnp.int32)
        key_pos = first_row - WIN + jnp.arange(span_rows + 2 * WIN, dtype=jnp.int32)
        allowed = (jnp.abs(key_pos[None, :] - query_pos[:, None]) <= WIN) & (key_docs[None, :] == query_docs[:, None])
        masked = jnp.where(allowed, scores, -1e+30)
        row_max = jnp.maximum(masked.max(-1, keepdims=True), sink_logit)
        exp_scores = jnp.where(allowed, jnp.exp(masked - row_max), 0.0)
        total_mass = exp_scores.sum(-1, keepdims=True) + jnp.exp(sink_logit - row_max)
        weights = (exp_scores / total_mass).astype(jnp.bfloat16).astype(jnp.float32)
        outcome = jnp.einsum('hgqk,khd->qhgd', weights, kv_span[..., HD:])
        return outcome.astype(jnp.bfloat16).reshape(span_rows, HQ * HD)
    attended = lax.map(one_span, jnp.arange(span_count, dtype=jnp.int32))
    return attended.reshape(TOKENS, HQ * HD)

def expert_apply(rows_in, gate_w, up_w, down_w):
    gate = jnp.dot(rows_in, gate_w, preferred_element_type=jnp.float32)
    upper = jnp.dot(rows_in, up_w, preferred_element_type=jnp.float32)
    expert_hidden = (jax.nn.silu(gate) * upper).astype(jnp.bfloat16)
    return jnp.dot(expert_hidden, down_w, preferred_element_type=jnp.float32).astype(jnp.bfloat16)

def reference(queries, keys_values, doc_ids, head_sink, out_weight, hidden_in, norm_gain, expert_gate, expert_up, expert_down, routes, route_weight):
    attended = attend_all(queries, keys_values, doc_ids, head_sink)
    projected = jnp.dot(attended, out_weight, preferred_element_type=jnp.float32)
    mid = (hidden_in.astype(jnp.float32) + projected).astype(jnp.bfloat16)
    mid_wide = mid.astype(jnp.float32)
    normed = (mid_wide * lax.rsqrt(lax.optimization_barrier(jnp.mean(mid_wide * mid_wide, axis=-1, keepdims=True)) + 1e-06) * norm_gain.astype(jnp.float32)).astype(jnp.bfloat16)
    local_rows = TOK_DEV // N_TP
    flat_routes = routes.reshape(EXPERTS, local_rows * TOPK)
    one_hot = (flat_routes[..., None] == jnp.arange(EXPERTS, dtype=jnp.int32)).astype(jnp.int32)
    slot_rank = (jnp.cumsum(one_hot, axis=1) * one_hot).sum(-1) - 1
    owner_block = jnp.arange(EXPERTS, dtype=jnp.int32)[:, None]
    slot_index = (flat_routes * (EXPERTS * CAP) + owner_block * CAP + slot_rank).reshape(-1).astype(jnp.int32)
    repeated = jnp.repeat(normed, TOPK, axis=0)
    buffer_rows = jnp.zeros((EXPERTS * EXPERTS * CAP, D), jnp.bfloat16).at[slot_index].set(repeated)

    def per_expert(pieces):
        return expert_apply(pieces[0], pieces[1], pieces[2], pieces[3])
    results = lax.map(per_expert, (buffer_rows.reshape(EXPERTS, EXPERTS * CAP, D), expert_gate, expert_up, expert_down))
    picked = results.reshape(-1, D)[slot_index].astype(jnp.float32).reshape(TOKENS, TOPK, D)
    mixture = lax.optimization_barrier(jnp.sum(picked * route_weight.astype(jnp.float32)[..., None], axis=1))
    return (mid_wide + mixture).astype(jnp.bfloat16)
```

```python
import jax
import jax.numpy as jnp
from jax import lax
from jax.sharding import Mesh, PartitionSpec as P

HD = 64
WIN = 128
BF = jnp.bfloat16
F32 = jnp.float32
SP = ("half", "rest")
GROUP = ("rest", "tp")
ALL = ("half", "rest", "tp")
SWAP = [(0, 1), (1, 0)]


def with_halo(cells, width):
    count = lax.axis_size(SP)
    head = lax.slice_in_dim(cells, 0, width, axis=0)
    tail = lax.slice_in_dim(cells, cells.shape[0] - width, cells.shape[0], axis=0)
    return jnp.concatenate(
        [
            lax.ppermute(tail, SP, [(i, i + 1) for i in range(count - 1)]),
            cells,
            lax.ppermute(head, SP, [(i + 1, i) for i in range(count - 1)]),
        ],
        axis=0,
    )


def attention(queries, keys_values, doc_ids, head_sink):
    tok_here = queries.shape[0]
    heads_here = head_sink.shape[0]
    kv_here = keys_values.shape[1]
    group = heads_here // kv_here
    head_dim = keys_values.shape[2] // 2
    kv_ext, docs_ext = with_halo(keys_values, WIN), with_halo(doc_ids, WIN)
    offset = lax.axis_index(SP) * tok_here
    seq_total = lax.axis_size(SP) * tok_here
    sink_logit = head_sink.reshape(kv_here, group)[:, :, None, None]
    q_span = queries.reshape(tok_here, kv_here, group, head_dim)
    scores = jnp.einsum(
        "qhgd,khd->hgqk", q_span, kv_ext[..., :head_dim], preferred_element_type=F32
    ) * HD ** (-0.5)
    query_pos = offset + jnp.arange(tok_here, dtype=jnp.int32)
    key_pos = offset - WIN + jnp.arange(tok_here + 2 * WIN, dtype=jnp.int32)
    inside = (key_pos >= 0) & (key_pos < seq_total)
    allowed = (
        (jnp.abs(key_pos[None, :] - query_pos[:, None]) <= WIN)
        & inside[None, :]
        & (docs_ext[None, :] == doc_ids[:, None])
    )
    masked = jnp.where(allowed, scores, -1e30)
    row_max = jnp.maximum(masked.max(-1, keepdims=True), sink_logit)
    exp_scores = jnp.where(allowed, jnp.exp(masked - row_max), 0.0)
    total_mass = exp_scores.sum(-1, keepdims=True) + jnp.exp(sink_logit - row_max)
    weights = (exp_scores / total_mass).astype(BF)
    outcome = jnp.einsum(
        "hgqk,khd->qhgd", weights, kv_ext[..., head_dim:], preferred_element_type=F32
    )
    return outcome.astype(BF).reshape(tok_here, heads_here * head_dim)


def slot_maps(routes, route_weight, first, experts, capacity):
    tokens = routes.shape[0]
    names = first + jnp.arange(experts, dtype=jnp.int32)
    hits = routes.T[None, :, :] == names[:, None, None]
    named = hits.any(1)
    weight = jnp.where(hits, route_weight.T[None], 0.0).sum(1)
    at = jnp.arange(tokens, dtype=jnp.int32)
    earlier = (at[:, None] < at[None, :]).astype(BF)
    rank = jnp.dot(named.astype(BF), earlier, preferred_element_type=F32)
    rank = jnp.where(named, rank, -1.0).astype(jnp.int32)
    slots = jnp.arange(capacity, dtype=jnp.int32)
    pick = rank[:, None, :] == slots[None, :, None]
    mix = jnp.where(pick, weight[:, None, :], 0.0)
    shape = (experts * capacity, tokens)
    return pick.astype(BF).reshape(shape), mix.reshape(shape)


def exchange(rows, experts):
    cut = rows.reshape(experts, -1, rows.shape[-1])
    return lax.all_to_all(cut, GROUP, split_axis=0, concat_axis=0, tiled=True).reshape(rows.shape)


def dispatch(pick, normed, experts):
    rows = jnp.dot(pick, normed, preferred_element_type=F32).astype(BF)
    return exchange(rows, experts)


def expert_rows(rows, gate_w, up_w, down_w):
    gate = jnp.dot(rows, gate_w, preferred_element_type=F32)
    upper = jnp.dot(rows, up_w, preferred_element_type=F32)
    hidden = (jax.nn.silu(gate) * upper).astype(BF)
    return jnp.dot(hidden, down_w, preferred_element_type=F32).astype(BF)


def combine(mix, rows):
    high = mix.astype(BF)
    low = (mix - high.astype(F32)).astype(BF)

    def part(m):
        return lax.dot_general(m, rows, (((0,), (0,)), ((), ())), preferred_element_type=F32)

    return part(high) + part(low)


def shards(
    queries,
    keys_values,
    doc_ids,
    head_sink,
    out_weight,
    hidden_in,
    norm_gain,
    expert_gate,
    expert_up,
    expert_down,
    routes,
    route_weight,
):
    attended = attention(queries, keys_values, doc_ids, head_sink)
    gathered = lax.all_to_all(attended, "tp", split_axis=0, concat_axis=1, tiled=True)
    projected = jnp.dot(gathered, out_weight, preferred_element_type=F32)
    mid = (hidden_in.astype(F32) + projected).astype(BF)
    mid_wide = mid.astype(F32)
    normed = (
        mid_wide
        * lax.rsqrt(jnp.mean(mid_wide * mid_wide, axis=-1, keepdims=True) + 1e-06)
        * norm_gain
    ).astype(BF)

    experts = lax.axis_size(GROUP)
    capacity = 2 * routes.shape[0] * routes.shape[1] // (2 * experts)
    first = lax.axis_index("half") * experts
    routes_far = lax.ppermute(routes, "half", SWAP)
    weight_far = lax.ppermute(route_weight, "half", SWAP)
    normed_far = lax.ppermute(normed, "half", SWAP)
    pick_near, mix_near = slot_maps(routes, route_weight, first, experts, capacity)
    pick_far, mix_far = slot_maps(routes_far, weight_far, first, experts, capacity)
    weights = (expert_gate[0], expert_up[0], expert_down[0])
    rows_near = expert_rows(dispatch(pick_near, normed, experts), *weights)
    rows_far = expert_rows(dispatch(pick_far, normed_far, experts), *weights)
    share_far = combine(mix_far, exchange(rows_far, experts)).astype(BF)
    share_back = lax.ppermute(share_far, "half", SWAP)
    share_near = combine(mix_near, exchange(rows_near, experts))
    return (mid.astype(F32) + share_near + share_back.astype(F32)).astype(BF)


def solution(mesh):
    sp, tp = mesh.shape["sp"], mesh.shape["tp"]
    halves = Mesh(mesh.devices.reshape(2, sp // 2, tp), ALL)
    placed = (
        P(SP, "tp"),
        P(SP, "tp", None),
        P(SP),
        P("tp"),
        P(),
        P(ALL, None),
        P(),
        P(ALL, None, None),
        P(ALL, None, None),
        P(ALL, None, None),
        P(ALL, None),
        P(ALL, None),
    )
    return jax.shard_map(
        shards, mesh=halves, in_specs=placed, out_specs=P(ALL, None), check_vma=False
    )
```
